32 devices in a mesh: ep: 16 (over z, x, core), tp: 2 (over y).
Axes of the slice: x: 2, y: 2, z: 4, core: 2. Of those that a mesh axis runs over, the one named last changes fastest.
Arguments:
- hidden_in: bfloat16 [256, 1024], P('ep', 'tp'), may hold values from -40 to 40
- norm_gain_attn: float32 [1024], replicated, may hold values from 0.1 to 1.9
- query_weight: bfloat16 [1024, 512], P(None, 'tp'), may hold values from -0.1875 to 0.1875
- key_weight: bfloat16 [1024, 512], P(None, 'tp'), may hold values from -0.1875 to 0.1875
- value_weight: bfloat16 [1024, 512], P(None, 'tp'), may hold values from -0.1875 to 0.1875
- query_gain: float32 [128], replicated, may hold values from 1 to 1.6
- key_gain: float32 [128], replicated, may hold values from 1 to 1.6
- lambda_head: float32 [4], P('tp'), may hold values from 0.3 to 0.8
- sub_gain: float32 [128], replicated, may hold values from 0.1 to 1.9
- out_weight: bfloat16 [512, 1024], P('tp'), may hold values from -0.25 to 0.25
- cache_key: bfloat16 [256, 256, 512], P('ep', None, 'tp'), may hold values from -8 to 8
- cache_value: bfloat16 [256, 256, 512], P('ep', None, 'tp'), may hold values from -6 to 6
- lengths: int32 [256], P('ep'), may hold values from 1 to 256
- norm_gain_mix: float32 [1024], P('tp'), may hold values from 0.1 to 1.9
- route_ids: int32 [256, 6], P('ep'), may hold values from 0 to 15, all different within a row; in each aligned block of 16 rows (0 to 15, 16 to 31, ...) at most 12 rows name the same one
- route_logits: float32 [256, 6], P('ep'), may hold values from -4 to 4
- expert_gate: bfloat16 [16, 1024, 1024], P('ep', None, 'tp'), may hold values from -0.5 to 0.5
- expert_up: bfloat16 [16, 1024, 1024], P('ep', None, 'tp'), may hold values from -0.5 to 0.5
- expert_down: bfloat16 [16, 1024, 1024], P('ep', 'tp'), may hold values from -0.046875 to 0.046875
- dense_gate: bfloat16 [1024, 2048], P('tp', 'ep'), may hold values from -0.1875 to 0.1875
- dense_up: bfloat16 [1024, 2048], P('tp', 'ep'), may hold values from -0.1875 to 0.1875
- dense_down: bfloat16 [2048, 1024], P('ep', 'tp'), may hold values from -0.125 to 0.125
- branch_gate: float32 [1024], P('tp'), may hold values from -0.1875 to 0.1875
Outputs:
- layer_out: bfloat16 [256, 1024], P('ep', 'tp')
- key_rows: bfloat16 [256, 512], P('ep', 'tp')
- value_rows: bfloat16 [256, 512], P('ep', 'tp')
The draws below stay inside these ranges and needn't reach their ends.
Inputs may be any that keep to these rules, and one draw needn't show every extreme that they name: `route_ids`: each row names 6 different experts. Among the rows of one index of ep (aligned blocks of 16 rows) no expert is named by more than 12 rows, and in some blocks one expert is named by exactly 12.
All inputs are finite; a program needn't handle non-finite values.
Results may differ from the reference program's by a relative error of at most 0.0075.
Values may be sent and summed in bfloat16 or wider, within the bound.
A program may use at most 64 MiB of HBM per device.

```python
import math
from functools import partial
import jax
import jax.numpy as jnp
import numpy as np
from jax import lax

D = 1024
HEADS = 4
QK = 64
VAL = 128
FF = 1024
DENSE = 2048
TOPK = 6
SEQ_GRP = 16
CACHE = 256
EXPERTS = 16
TOKENS = 256
CAP = 12
N_EP = 16


def draw_hidden_in(key, part):
    row_key, entry_key = jax.random.split(jax.random.fold_in(key, 11))
    position = jnp.arange(D, dtype=jnp.float32) / D
    column_scale = 0.5 * 3.0 ** position
    entries = jnp.clip(jax.random.normal(entry_key, (TOKENS, D), jnp.float32), -4.0, 4.0)
    row_scale = jnp.exp(jax.random.uniform(row_key, (TOKENS, 1), jnp.float32, -0.7, 1.2))
    return (entries * row_scale * column_scale[None, :]).astype(jnp.bfloat16)


def plant(values, rng, smallest, high):
    spot = [jax.random.randint(jax.random.fold_in(rng, axis), (), 0, length) for axis, length in enumerate(values.shape)]
    widest = values.shape.index(max(values.shape))
    beside = spot[:widest] + [(spot[widest] + 1) % values.shape[widest]] + spot[widest + 1:]
    return values.at[tuple(spot)].set(smallest).at[tuple(beside)].set(high)


def levels(rng, extent, shards, smallest, top_value):
    def one(axis_at, parts):
        draws = jax.random.uniform(jax.random.fold_in(jax.random.fold_in(rng, 6), axis_at), (parts,), jnp.float32, smallest / len(shards), top_value / len(shards))
        return jnp.repeat(jnp.exp(draws), extent[axis_at] // parts).reshape((-1,) + (1,) * (len(extent) - axis_at - 1))

    level = one(*shards[0])
    for cut in shards[1:]:
        level = level * one(*cut)
    return level


def assign_block(own_key, own, number, rows, amount, top, most, slope):
    ranking = jax.random.permutation(own_key, amount)
    packed, common = portions_of(amount, rows * top, most, slope, True), portions_of(amount, rows * top, most, slope, False)
    places = jnp.arange(amount)

    def named(sizes, offset_by):
        used = int((sizes > 0).sum())
        fixed = max(1, used // 4)
        shifted = fixed + (places - fixed + offset_by * (used - fixed)) % max(1, amount - fixed)
        return jnp.zeros((amount,), jnp.int32).at[ranking[jnp.where(places < fixed, places, shifted)]].set(jnp.asarray(sizes, jnp.int32))

    sizes = jnp.where(number % 4 == 0, named(packed, number // 4), named(common, number - number // 4 - 1))
    mixed = jax.random.permutation(jax.random.fold_in(own, 3), amount)
    donor, sink = mixed[0:amount // 2 * 2:2], mixed[1:amount // 2 * 2:2]
    margin = jnp.minimum(sizes[donor] - 1, most - sizes[sink]) // 2
    margin = jnp.where((donor == ranking[0]) | (sink == ranking[0]) | (sizes[sink] == 0), 0, jnp.maximum(margin, 0))
    shifted = jax.random.randint(jax.random.fold_in(own, 4), (amount // 2,), 0, 1 << 20) % (margin + 1)
    sizes = sizes.at[donor].add(-shifted).at[sink].add(shifted)
    items = jnp.searchsorted(jnp.cumsum(sizes), jnp.arange(rows * top), side="right").astype(jnp.int32)
    table = items.reshape(top, rows).T
    table = table[jax.random.permutation(jax.random.fold_in(own, 1), rows)]
    offset_by = jax.random.randint(jax.random.fold_in(own, 2), (rows, 1), 0, top)
    return jnp.take_along_axis(table, (jnp.arange(top)[None, :] + offset_by) % top, axis=1)


def portions_of(amount, total, limit, slope, full):
    portions = [(1 << 20) // math.isqrt(rank ** slope) + 1 for rank in range(1, amount + 1)]
    largest = limit if full else min(limit, max(-(-total // amount), total * portions[0] // sum(portions)))
    least = 1 if total - largest >= amount - 1 else 0
    holding, rest = [largest] + [least] * (amount - 1), total - largest - least * (amount - 1)
    while rest > 0:
        candidates = [i for i in range(1, amount) if holding[i] < largest] or [i for i in range(1, amount) if holding[i] < limit]
        pool, left = sum([portions[i] for i in candidates]), rest
        for i in candidates:
            addition = min(limit - holding[i], max(1, left * portions[i] // pool), rest)
            holding[i] = holding[i] + addition
            rest = rest - addition
    return np.array(holding)


def normal_values(stream_key, dims, spread, reach, cuts=(), kind=jnp.bfloat16):
    gain = levels(stream_key, dims, cuts, -0.22, 0.18) if cuts else 1.0
    drawn = jax.random.normal(stream_key, dims, jnp.float32) * spread * gain
    return jnp.minimum(jnp.maximum(drawn, -reach), reach).astype(kind)


def setup_inputs(seed: int = 0) -> dict:
    key_of = jax.random.split(jax.random.key(seed), 24)
    hidden_in = draw_hidden_in(jax.random.fold_in(key_of[23], 71), 0)
    norm_gain_attn = jnp.clip(1.0 + 0.18 * jax.random.normal(key_of[1], (D,), jnp.float32), 0.1, 1.9)
    query_weight = normal_values(key_of[2], (D, HEADS * 2 * QK), D ** -0.5, 0.1875, ((1, 2),))
    key_weight = normal_values(key_of[3], (D, HEADS * 2 * QK), D ** -0.5, 0.1875, ((1, 2),))
    value_weight = normal_values(key_of[4], (D, HEADS * VAL), D ** -0.5, 0.1875, ((1, 2),))
    query_gain = jnp.clip(jax.random.uniform(key_of[5], (2 * QK,), jnp.float32, 1.0, 1.6), 1.0, 1.6)
    key_gain = jnp.clip(jax.random.uniform(key_of[6], (2 * QK,), jnp.float32, 1.0, 1.6), 1.0, 1.6)
    lambda_head = jnp.clip(0.3 + 0.5 * jax.random.uniform(key_of[7], (HEADS,), jnp.float32) ** levels(key_of[7], (HEADS,), ((0, 2),), -0.2, 0.2), 0.3, 0.8)
    sub_gain = jnp.clip(1.0 + 0.18 * jax.random.normal(key_of[8], (VAL,), jnp.float32), 0.1, 1.9)
    out_weight = normal_values(key_of[9], (HEADS * VAL, D), (HEADS * VAL) ** -0.5, 0.25, ((0, 2),))
    cache_key = normal_values(key_of[10], (TOKENS, CACHE, HEADS * 2 * QK), 1.25, 8.0, ((0, 16), (2, 2)))
    cache_value = normal_values(key_of[11], (TOKENS, CACHE, HEADS * VAL), 1.0, 6.0, ((0, 16), (2, 2)))
    lengths = plant(jax.random.randint(key_of[12], (TOKENS,), 1, CACHE + 1), jax.random.fold_in(key_of[12], 1), 1, CACHE).astype(jnp.int32)
    norm_gain_mix = jnp.clip(1.0 + 0.18 * jax.random.normal(key_of[13], (D,), jnp.float32), 0.1, 1.9)
    route_ids_keys = jax.random.split(jax.random.fold_in(key_of[14], 1), TOKENS // SEQ_GRP)
    route_ids_turns = jax.random.permutation(jax.random.fold_in(key_of[14], 3), TOKENS // SEQ_GRP)
    route_ids = jax.vmap(lambda own, number: assign_block(jax.random.fold_in(key_of[14], 2), own, number, SEQ_GRP, EXPERTS, TOPK, CAP, 1))(route_ids_keys, route_ids_turns).reshape((TOKENS, TOPK))
    route_logits = normal_values(key_of[15], (TOKENS, TOPK), 1.0, 4.0, ((0, 16),), jnp.float32)
    expert_gate = normal_values(key_of[16], (EXPERTS, D, FF), (D // 9) ** -0.5, 0.5, ((0, 16), (2, 2)))
    expert_up = normal_values(key_of[17], (EXPERTS, D, FF), (D // 9) ** -0.5, 0.5, ((0, 16), (2, 2)))
    expert_down = normal_values(key_of[18], (EXPERTS, FF, D), (16 * FF) ** -0.5, 0.046875, ((0, 16), (1, 2)))
    dense_gate = normal_values(key_of[19], (D, DENSE), D ** -0.5, 0.1875, ((0, 2), (1, 16)))
    dense_up = normal_values(key_of[20], (D, DENSE), D ** -0.5, 0.1875, ((0, 2), (1, 16)))
    dense_down = normal_values(key_of[21], (DENSE, D), DENSE ** -0.5, 0.125, ((0, 16), (1, 2)))
    branch_gate = normal_values(key_of[22], (D,), D ** -0.5, 0.1875, ((0, 2),), jnp.float32)
    return {"hidden_in": hidden_in, "norm_gain_attn": norm_gain_attn, "query_weight": query_weight, "key_weight": key_weight, "value_weight": value_weight, "query_gain": query_gain, "key_gain": key_gain, "lambda_head": lambda_head, "sub_gain": sub_gain, "out_weight": out_weight, "cache_key": cache_key, "cache_value": cache_value, "lengths": lengths, "norm_gain_mix": norm_gain_mix, "route_ids": route_ids, "route_logits": route_logits, "expert_gate": expert_gate, "expert_up": expert_up, "expert_down": expert_down, "dense_gate": dense_gate, "dense_up": dense_up, "dense_down": dense_down, "branch_gate": branch_gate}


EPSILON = 1e-06
CLAMP_LIMIT = 7.0
SWISH_ALPHA = 1.702
OUT_SCALE = 0.2 + 0.6 * math.exp(-0.6)

def rms_scale(values, scale_gain):
    mean_square = lax.optimization_barrier(jnp.mean(values * values, axis=-1, keepdims=True))
    return values * lax.rsqrt(mean_square + EPSILON) * scale_gain

def clamped_unit(gate_pre, up_pre):
    gate_cut = jnp.minimum(gate_pre, CLAMP_LIMIT)
    up_cut = jnp.clip(up_pre, -CLAMP_LIMIT, CLAMP_LIMIT)
    return (up_cut + 1.0) * gate_cut * jax.nn.sigmoid(SWISH_ALPHA * gate_cut)

def attend_block(block, lambda_head, sub_gain):
    query_rows, key_new, value_new, key_cache, value_cache, length_rows = block
    seq_count = query_rows.shape[0]
    scale_factor = QK ** (-0.5)
    query_float = query_rows.astype(jnp.float32)
    key_past = key_cache.astype(jnp.float32).reshape(seq_count, CACHE, HEADS, 2, QK)
    past_score = jnp.einsum('shmd,sjhmd->shmj', query_float, key_past) * scale_factor
    own_score = lax.optimization_barrier(jnp.sum(query_float * key_new.astype(jnp.float32), axis=-1)) * scale_factor
    valid_mask = lax.iota(jnp.int32, CACHE)[None, :] < length_rows[:, None]
    past_exp = jnp.where(valid_mask[:, None, None, :], jnp.exp(past_score), 0.0)
    own_exp = jnp.exp(own_score)
    denominator = lax.optimization_barrier(jnp.sum(past_exp, axis=-1)) + own_exp
    past_prob = past_exp / denominator[..., None]
    own_prob = own_exp / denominator
    weight_past = (past_prob[:, :, 0] - lambda_head[None, :, None] * past_prob[:, :, 1]).astype(jnp.bfloat16)
    weight_own = (own_prob[:, :, 0] - lambda_head[None, :] * own_prob[:, :, 1]).astype(jnp.bfloat16)
    value_past = value_cache.astype(jnp.float32).reshape(seq_count, CACHE, HEADS, VAL)
    head_mix = jnp.einsum('shj,sjhe->she', weight_past.astype(jnp.float32), value_past)
    head_mix = head_mix + weight_own.astype(jnp.float32)[..., None] * value_new.astype(jnp.float32)
    head_out = (rms_scale(head_mix, sub_gain) * OUT_SCALE).astype(jnp.bfloat16)
    return head_out.reshape(seq_count, HEADS * VAL)

def expert_routes(mix_rows, route_ids, expert_gate, expert_up, expert_down):
    flat_ids = route_ids.reshape(-1).astype(jnp.int32)
    route_total = flat_ids.shape[0]
    most_rows = N_EP * CAP

    def one_expert(carried, index):
        order = jnp.argsort(jnp.where(flat_ids == index, 0, 1).astype(jnp.int32), stable=True)[:most_rows]
        order = order.astype(jnp.int32)
        chosen = flat_ids[order] == index
        token_rows = mix_rows[order // TOPK]
        gate_pre = jnp.dot(token_rows, expert_gate[index], preferred_element_type=jnp.float32)
        up_pre = jnp.dot(token_rows, expert_up[index], preferred_element_type=jnp.float32)
        activation = clamped_unit(gate_pre, up_pre).astype(jnp.bfloat16)
        result = jnp.dot(activation, expert_down[index], preferred_element_type=jnp.float32).astype(jnp.bfloat16)
        result = lax.optimization_barrier(result).astype(jnp.float32)
        result = jnp.where(chosen[:, None], result, 0.0)
        return (carried.at[order].add(result), None)
    start_rows = jnp.zeros((route_total, D), jnp.float32)
    routed_rows, _ = lax.scan(one_expert, start_rows, jnp.arange(EXPERTS, dtype=jnp.int32))
    return routed_rows

def reference(hidden_in, norm_gain_attn, query_weight, key_weight, value_weight, query_gain, key_gain, lambda_head, sub_gain, out_weight, cache_key, cache_value, lengths, norm_gain_mix, route_ids, route_logits, expert_gate, expert_up, expert_down, dense_gate, dense_up, dense_down, branch_gate):
    normed = rms_scale(hidden_in.astype(jnp.float32), norm_gain_attn).astype(jnp.bfloat16)
    query_pre = jnp.dot(normed, query_weight, preferred_element_type=jnp.float32).reshape(TOKENS, HEADS, 2, QK)
    query_rows = rms_scale(query_pre, query_gain.reshape(2, QK)).astype(jnp.bfloat16)
    key_pre = jnp.dot(normed, key_weight, preferred_element_type=jnp.float32).reshape(TOKENS, HEADS, 2, QK)
    key_rows = rms_scale(key_pre, key_gain.reshape(2, QK)).astype(jnp.bfloat16)
    value_rows = jnp.dot(normed, value_weight, preferred_element_type=jnp.float32).astype(jnp.bfloat16)
    blocks = (query_rows.reshape(N_EP, SEQ_GRP, HEADS, 2, QK), key_rows.reshape(N_EP, SEQ_GRP, HEADS, 2, QK), value_rows.reshape(N_EP, SEQ_GRP, HEADS, VAL), cache_key.reshape(N_EP, SEQ_GRP, CACHE, HEADS * 2 * QK), cache_value.reshape(N_EP, SEQ_GRP, CACHE, HEADS * VAL), lengths.reshape(N_EP, SEQ_GRP))
    head_out = lax.map(partial(attend_block, lambda_head=lambda_head, sub_gain=sub_gain), blocks)
    head_out = head_out.reshape(TOKENS, HEADS * VAL)
    attn_out = jnp.dot(head_out, out_weight, preferred_element_type=jnp.float32)
    residual = hidden_in.astype(jnp.float32) + attn_out
    inverse = lax.rsqrt(lax.optimization_barrier(jnp.mean(residual * residual, axis=1, keepdims=True)) + EPSILON)
    mix_float = residual * inverse * norm_gain_mix
    mix_rows = mix_float.astype(jnp.bfloat16)
    branch_weight = jax.nn.sigmoid(lax.optimization_barrier(jnp.sum(mix_float * branch_gate, axis=1, keepdims=True)))
    route_weight = jax.nn.softmax(route_logits, axis=1)
    routed_rows = expert_routes(mix_rows, route_ids, expert_gate, expert_up, expert_down)
    routed = lax.optimization_barrier(jnp.sum(routed_rows.reshape(TOKENS, TOPK, D) * route_weight[:, :, None], axis=1))
    dense_gate_pre = jnp.dot(mix_rows, dense_gate, preferred_element_type=jnp.float32)
    dense_up_pre = jnp.dot(mix_rows, dense_up, preferred_element_type=jnp.float32)
    dense_act = (jax.nn.silu(dense_gate_pre) * dense_up_pre).astype(jnp.bfloat16)
    dense_result = jnp.dot(dense_act, dense_down, preferred_element_type=jnp.float32)
    layer_out = (residual + routed + branch_weight * dense_result).astype(jnp.bfloat16)
    return (layer_out, key_rows.reshape(TOKENS, HEADS * 2 * QK), value_rows)
```

```python
import functools
import math

import jax
import jax.numpy as jnp
from jax import lax
from jax.experimental import pallas as pl
from jax.experimental.pallas import tpu as pltpu
from jax.sharding import PartitionSpec as P

EPSILON = 1e-06
CLAMP_LIMIT = 7.0
SWISH_ALPHA = 1.702
OUT_SCALE = 0.2 + 0.6 * math.exp(-0.6)
F32 = jnp.float32
BF16 = jnp.bfloat16
MESH = pl.DeviceIdType.MESH


def dot(a, b):
    return jnp.dot(a, b, preferred_element_type=F32)


def group_rms(values, gain, group):
    lane = lax.broadcasted_iota(jnp.int32, values.shape, 1)
    squares = values * values
    scale = jnp.zeros_like(values)
    for g in range(values.shape[1] // group):
        inside = (lane >= g * group) & (lane < (g + 1) * group)
        total = jnp.sum(jnp.where(inside, squares, 0.0), axis=1, keepdims=True)
        scale = jnp.where(inside, lax.rsqrt(total / group + EPSILON), scale)
    return values * scale * gain


def layer_kernel(
    n_ep,
    n_tp,
    lam_ref,
    len_ref,
    hid_ref,
    gain_attn_ref,
    qg_ref,
    kg_ref,
    sub_ref,
    gain_mix_ref,
    branch_ref,
    ids_ref,
    logits_ref,
    wq_hbm,
    wk_hbm,
    wv_hbm,
    wo_hbm,
    ck_hbm,
    cv_hbm,
    eg_hbm,
    eu_hbm,
    ed_hbm,
    dg_hbm,
    du_hbm,
    dd_hbm,
    out_ref,
    key_ref,
    val_ref,
    wq,
    wk,
    wv,
    wo,
    ck,
    cv,
    eg,
    eu,
    ed,
    dgbuf,
    dubuf,
    dd,
    hbuf,
    gbuf,
    bbuf,
    vrow,
    hout,
    res,
    abuf,
    gath,
    ybuf,
    ysend,
    pbuf,
    sbuf,
    rbuf,
    lsem,
    tp_send,
    tp_recv,
    g_send,
    f_send,
    g_recv,
    p_sem,
    r_send,
    r_recv,
):
    e = lax.axis_index("ep")
    t = lax.axis_index("tp")
    chips = n_ep // 2
    chip = lax.div(e, 2)
    core = lax.rem(e, 2)
    sib = chip * 2 + (1 - core)
    n_all = chips * n_tp
    rows, half = hid_ref.shape
    width = half * n_tp

    loads = []
    for i, (src, dst) in enumerate(
        [
            (wq_hbm, wq),
            (wk_hbm, wk),
            (wv_hbm, wv),
            (ck_hbm, ck),
            (cv_hbm, cv),
            (wo_hbm, wo),
            (dg_hbm, dgbuf.at[t]),
            (du_hbm, dubuf.at[t]),
            (eg_hbm.at[0], eg),
            (eu_hbm.at[0], eu),
            (ed_hbm.at[0], ed),
            (dd_hbm, dd),
        ]
    ):
        copy = pltpu.make_async_copy(src, dst, lsem.at[i])
        copy.start()
        loads.append(copy)

    barrier = pltpu.get_barrier_semaphore()
    me = t * chips + chip

    def greet(i, carry):
        other = lax.rem(me + i, n_all)
        pl.semaphore_signal(
            barrier,
            inc=1,
            device_id={"ep": lax.rem(other, chips) * 2 + core, "tp": lax.div(other, chips)},
            device_id_type=MESH,
        )
        return carry

    lax.fori_loop(1, n_all, greet, 0)
    pl.semaphore_signal(barrier, inc=1, device_id={"ep": sib, "tp": t}, device_id_type=MESH)

    hbuf[t] = hid_ref[...]
    gbuf[t] = gain_mix_ref[...]
    bbuf[t] = branch_ref[...]

    ext = gath.shape[2] - width
    logits = logits_ref[...]
    top = logits - jnp.max(logits, axis=1, keepdims=True)
    expo = jnp.exp(top)
    route = expo / jnp.sum(expo, axis=1, keepdims=True)
    ids = ids_ref[...]
    lane = lax.broadcasted_iota(jnp.int32, (rows, ext), 1)
    first = lane <= n_ep
    lane_id = jnp.where(first, lane, lane - (n_ep + 1))
    table = jnp.zeros((rows, ext), F32)
    for k in range(ids.shape[1]):
        table = table + jnp.where(lane_id == ids[:, k : k + 1], route[:, k : k + 1], 0.0)

    pl.semaphore_wait(barrier, n_all)

    def tp_copies(kind, src, dst_ref):
        sends = []
        for d in range(1, n_tp):
            peer = lax.rem(t + d, n_tp)
            copy = pltpu.make_async_remote_copy(
                src_ref=src,
                dst_ref=dst_ref.at[t],
                send_sem=tp_send.at[kind, d - 1],
                recv_sem=tp_recv.at[kind, t],
                device_id={"ep": e, "tp": peer},
                device_id_type=MESH,
            )
            copy.start()
            sends.append(copy)
        return sends

    def tp_arrive(kind, src, dst_ref):
        for d in range(1, n_tp):
            peer = lax.rem(t + d, n_tp)
            pltpu.make_async_remote_copy(
                src_ref=src,
                dst_ref=dst_ref.at[peer],
                send_sem=tp_send.at[kind, d - 1],
                recv_sem=tp_recv.at[kind, peer],
                device_id={"ep": e, "tp": peer},
                device_id_type=MESH,
            ).wait_recv()

    pending = []
    pending += tp_copies(0, hid_ref, hbuf)
    pending += tp_copies(1, gain_mix_ref, gbuf)
    pending += tp_copies(2, branch_ref, bbuf)

    tp_arrive(0, hid_ref, hbuf)
    hidden = [hbuf[j].astype(F32) for j in range(n_tp)]
    square = sum(jnp.sum(h * h, axis=1, keepdims=True) for h in hidden)
    inverse = lax.rsqrt(square / width + EPSILON)
    normed = [
        (hidden[j] * inverse * gain_attn_ref[:, j * half : (j + 1) * half]).astype(BF16)
        for j in range(n_tp)
    ]

    def project(w):
        return sum(dot(normed[j], w[j * half : (j + 1) * half, :]) for j in range(n_tp))

    qk2 = qg_ref.shape[1]
    qk = qk2 // 2
    cols = wq.shape[1]
    heads = cols // qk2
    val = sub_ref.shape[1]
    q_gain = jnp.concatenate([qg_ref[...]] * heads, axis=1)
    k_gain = jnp.concatenate([kg_ref[...]] * heads, axis=1)
    sub_gain = jnp.concatenate([sub_ref[...]] * heads, axis=1)
    loads[0].wait()
    q_rows = group_rms(project(wq), q_gain, qk).astype(BF16).astype(F32)
    loads[1].wait()
    k_bf = group_rms(project(wk), k_gain, qk).astype(BF16)
    k_rows = k_bf.astype(F32)
    loads[2].wait()
    v_bf = project(wv).astype(BF16)
    key_ref[...] = k_bf
    val_ref[...] = v_bf
    vrow[...] = v_bf.astype(F32)

    qcol = lax.broadcasted_iota(jnp.int32, (16, cols), 1)
    qrow = lax.broadcasted_iota(jnp.int32, (16, cols), 0)
    inside = (qcol // qk) == (2 * (qrow % 8) + qrow // 8)
    vcol = lax.broadcasted_iota(jnp.int32, (8, heads * val), 1)
    vhead = lax.broadcasted_iota(jnp.int32, (8, heads * val), 0)
    own_head = (vcol // val) == vhead
    lrow = lax.broadcasted_iota(jnp.int32, (8, 1), 0)
    lam = jnp.zeros((8, 1), F32)
    for h in range(heads):
        lam = jnp.where(lrow == h, lam_ref[h], lam)
    factor = qk ** (-0.5)
    cache_len = ck.shape[1]
    pos = lax.broadcasted_iota(jnp.int32, (16, cache_len), 1)
    loads[3].wait()
    loads[4].wait()
    for s in range(rows):
        q_s = jnp.where(inside, q_rows[s : s + 1, :], 0.0)
        own = jnp.exp(jnp.sum(q_s * k_rows[s : s + 1, :], axis=1, keepdims=True) * factor)
        score = lax.dot_general(
            q_s.astype(BF16), ck[s], (((1,), (1,)), ((), ())), preferred_element_type=F32
        )
        past = jnp.where(pos < len_ref[s], jnp.exp(score * factor), 0.0)
        inv_den = 1.0 / (jnp.sum(past, axis=1, keepdims=True) + own)
        prob = past * inv_den
        own = own * inv_den
        weight = (prob[:8] - lam * prob[8:]).astype(BF16)
        weight_own = (own[:8] - lam * own[8:]).astype(BF16).astype(F32)
        mix = dot(weight, cv[s]) + weight_own * vrow[s : s + 1, :]
        mix = jnp.where(own_head, mix, 0.0)
        square = jnp.sum(mix * mix, axis=1, keepdims=True)
        mix = mix * lax.rsqrt(square / val + EPSILON) * sub_gain * OUT_SCALE
        hout[s : s + 1, :] = jnp.sum(mix, axis=0, keepdims=True)
    loads[5].wait()
    attn = dot(hout[...].astype(BF16), wo[...])
    abuf[t] = attn.astype(BF16)
    pending += tp_copies(3, abuf.at[t], abuf)
    loads[6].wait()
    loads[7].wait()
    pending += tp_copies(4, dgbuf.at[t], dgbuf)
    pending += tp_copies(5, dubuf.at[t], dubuf)
    tp_arrive(1, gain_mix_ref, gbuf)
    tp_arrive(2, branch_ref, bbuf)
    tp_arrive(3, abuf.at[t], abuf)

    for d in range(1, n_tp):
        attn = attn + abuf[lax.rem(t + d, n_tp)].astype(F32)
    slot = core * chips + chip
    square = jnp.zeros((rows, 1), F32)
    total = []
    for j in range(n_tp):
        r = hbuf[j].astype(F32) + attn[:, j * half : (j + 1) * half]
        res[j] = r
        total.append(r)
        square = square + jnp.sum(r * r, axis=1, keepdims=True)
    inverse = lax.rsqrt(square / width + EPSILON)
    logit = jnp.zeros((rows, 1), F32)
    for j in range(n_tp):
        m = total[j] * inverse * gbuf[j]
        logit = logit + jnp.sum(m * bbuf[j], axis=1, keepdims=True)
        gath[slot, :, j * half : (j + 1) * half] = m.astype(BF16)
    branch = 1.0 / (1.0 + jnp.exp(-logit))
    table = jnp.where(lane_id == n_ep, branch, table)
    high = table.astype(BF16).astype(F32)
    gath[slot, :, width:] = jnp.where(first, high, table - high).astype(BF16)

    def gather_copy(at, send, ep_to):
        return pltpu.make_async_remote_copy(
            src_ref=gath.at[at],
            dst_ref=gath.at[at],
            send_sem=send,
            recv_sem=g_recv.at[at],
            device_id={"ep": ep_to, "tp": t},
            device_id_type=MESH,
        )

    def scatter(i, carry):
        to = lax.rem(chip + i, chips)
        gather_copy(slot, g_send.at[i], to * 2 + core).start()
        return carry

    lax.fori_loop(1, chips, scatter, 0)
    gather_copy(slot, g_send.at[0], sib).start()

    def forward(i, carry):
        at = core * chips + lax.rem(chip + chips - i, chips)
        gather_copy(at, f_send.at[i], sib).wait_recv()
        gather_copy(at, f_send.at[i], sib).start()
        return carry

    lax.fori_loop(1, chips, forward, 0)

    for i in range(8, 12):
        loads[i].wait()
    tp_arrive(4, dgbuf.at[t], dgbuf)
    tp_arrive(5, dubuf.at[t], dubuf)

    def expert(par):
        x = gath[pl.ds(par * chips, chips), :, :].reshape(chips * rows, width + ext)
        tokens = x[:, :width]
        extra = x[:, width:].astype(F32)
        place = lax.broadcasted_iota(jnp.int32, extra.shape, 1)
        mine = (place == e) | (place == e + n_ep + 1)
        w_route = jnp.sum(jnp.where(mine, extra, 0.0), axis=1, keepdims=True)
        dense_at = (place == n_ep) | (place == 2 * n_ep + 1)
        w_dense = jnp.sum(jnp.where(dense_at, extra, 0.0), axis=1, keepdims=True)
        gate = jnp.minimum(dot(tokens, eg[...]), CLAMP_LIMIT)
        up = jnp.clip(dot(tokens, eu[...]), -CLAMP_LIMIT, CLAMP_LIMIT)
        act = ((up + 1.0) * gate / (1.0 + jnp.exp(-SWISH_ALPHA * gate))).astype(BF16)
        dg = sum(dot(tokens[:, j * half : (j + 1) * half], dgbuf[j]) for j in range(n_tp))
        du = sum(dot(tokens[:, j * half : (j + 1) * half], dubuf[j]) for j in range(n_tp))
        dact = (dg / (1.0 + jnp.exp(-dg)) * du).astype(BF16)
        dense = dot(dact, dd[...]) * w_dense
        parts = []
        for j in range(n_tp):
            y = dot(act, ed[:, j * half : (j + 1) * half]) * w_route
            parts.append((y + jnp.where(t == j, dense, 0.0)).reshape(chips, rows, half))
        return parts

    own_parts = expert(core)
    for j in range(n_tp):
        ybuf[j] = own_parts[j]

    def arrived(i, carry):
        at = (1 - core) * chips + i
        gather_copy(at, g_send.at[0], sib).wait_recv()
        return carry

    lax.fori_loop(0, chips, arrived, 0)
    sib_parts = expert(1 - core)
    for j in range(n_tp):
        ysend[j] = sib_parts[j].astype(BF16)
    pair = pltpu.make_async_remote_copy(
        src_ref=ysend,
        dst_ref=pbuf,
        send_sem=p_sem.at[0],
        recv_sem=p_sem.at[1],
        device_id={"ep": sib, "tp": t},
        device_id_type=MESH,
    )
    pair.start()
    pair.wait_recv()
    for j in range(n_tp):
        both = ybuf[j] + pbuf[j].astype(F32)
        sbuf[j] = both.astype(BF16)

    def result_copy(i, to_t, to_chip, from_t, from_chip):
        return pltpu.make_async_remote_copy(
            src_ref=sbuf.at[to_t, to_chip],
            dst_ref=rbuf.at[from_t, from_chip],
            send_sem=r_send.at[i],
            recv_sem=r_recv.at[from_t * chips + from_chip],
            device_id={"ep": to_chip * 2 + core, "tp": to_t},
            device_id_type=MESH,
        )

    def give(i, carry):
        to = lax.rem(me + i, n_all)
        result_copy(i, lax.div(to, chips), lax.rem(to, chips), t, chip).start()
        return carry

    lax.fori_loop(1, n_all, give, 0)
    final = res[t] + ybuf[t, chip] + pbuf[t, chip].astype(F32)

    def take(i, total):
        src = lax.rem(me + n_all - i, n_all)
        src_t, src_chip = lax.div(src, chips), lax.rem(src, chips)
        result_copy(i, t, chip, src_t, src_chip).wait_recv()
        return total + rbuf[src_t, src_chip].astype(F32)

    final = lax.fori_loop(1, n_all, take, final)
    out_ref[...] = final.astype(BF16)

    for copy in pending:
        copy.wait_send()
    pair.wait_send()

    def drain_gather(i, carry):
        gather_copy(slot, g_send.at[i], sib).wait_send()
        return carry

    lax.fori_loop(0, chips, drain_gather, 0)

    def drain_forward(i, carry):
        gather_copy(slot, f_send.at[i], sib).wait_send()
        return carry

    lax.fori_loop(1, chips, drain_forward, 0)

    def drain_result(i, carry):
        to = lax.rem(me + i, n_all)
        result_copy(i, lax.div(to, chips), lax.rem(to, chips), t, chip).wait_send()
        return carry

    lax.fori_loop(1, n_all, drain_result, 0)


def body(
    n_ep,
    n_tp,
    hidden_in,
    norm_gain_attn,
    query_weight,
    key_weight,
    value_weight,
    query_gain,
    key_gain,
    lambda_head,
    sub_gain,
    out_weight,
    cache_key,
    cache_value,
    lengths,
    norm_gain_mix,
    route_ids,
    route_logits,
    expert_gate,
    expert_up,
    expert_down,
    dense_gate,
    dense_up,
    dense_down,
    branch_gate,
):
    rows, half = hidden_in.shape
    width = half * n_tp
    chips = n_ep // 2
    n_all = chips * n_tp
    ext = -(-2 * (n_ep + 1) // 128) * 128
    smem = pl.BlockSpec(memory_space=pltpu.SMEM)
    vmem = pl.BlockSpec(memory_space=pltpu.VMEM)
    hbm = pl.BlockSpec(memory_space=pl.ANY)
    dma = pltpu.SemaphoreType.DMA
    cols = query_weight.shape[1]
    vcols = value_weight.shape[1]
    block = (n_tp, chips, rows, half)
    scratch = [
        pltpu.VMEM(query_weight.shape, BF16),
        pltpu.VMEM(key_weight.shape, BF16),
        pltpu.VMEM(value_weight.shape, BF16),
        pltpu.VMEM(out_weight.shape, BF16),
        pltpu.VMEM(cache_key.shape, BF16),
        pltpu.VMEM(cache_value.shape, BF16),
        pltpu.VMEM(expert_gate.shape[1:], BF16),
        pltpu.VMEM(expert_up.shape[1:], BF16),
        pltpu.VMEM(expert_down.shape[1:], BF16),
        pltpu.VMEM((n_tp,) + dense_gate.shape, BF16),
        pltpu.VMEM((n_tp,) + dense_up.shape, BF16),
        pltpu.VMEM(dense_down.shape, BF16),
        pltpu.VMEM((n_tp, rows, half), BF16),
        pltpu.VMEM((n_tp, 1, half), F32),
        pltpu.VMEM((n_tp, 1, half), F32),
        pltpu.VMEM((rows, vcols), F32),
        pltpu.VMEM((rows, vcols), F32),
        pltpu.VMEM((n_tp, rows, half), F32),
        pltpu.VMEM((n_tp, rows, width), BF16),
        pltpu.VMEM((n_ep, rows, width + ext), BF16),
        pltpu.VMEM(block, F32),
        pltpu.VMEM(block, BF16),
        pltpu.VMEM(block, BF16),
        pltpu.VMEM(block, BF16),
        pltpu.VMEM(block, BF16),
        dma((12,)),
        dma((6, n_tp)),
        dma((6, n_tp)),
        dma((chips,)),
        dma((chips,)),
        dma((n_ep,)),
        dma((2,)),
        dma((n_all,)),
        dma((n_all,)),
    ]
    return pl.pallas_call(
        functools.partial(layer_kernel, n_ep, n_tp),
        out_shape=(
            jax.ShapeDtypeStruct((rows, half), BF16),
            jax.ShapeDtypeStruct((rows, cols), BF16),
            jax.ShapeDtypeStruct((rows, vcols), BF16),
        ),
        in_specs=[smem] * 2 + [vmem] * 9 + [hbm] * 12,
        out_specs=(vmem, vmem, vmem),
        scratch_shapes=scratch,
        compiler_params=pltpu.CompilerParams(
            collective_id=0, has_side_effects=True, vmem_limit_bytes=56 * 1024 * 1024
        ),
    )(
        lambda_head,
        lengths,
        hidden_in,
        norm_gain_attn.reshape(1, -1),
        query_gain.reshape(1, -1),
        key_gain.reshape(1, -1),
        sub_gain.reshape(1, -1),
        norm_gain_mix.reshape(1, -1),
        branch_gate.reshape(1, -1),
        route_ids,
        route_logits,
        query_weight,
        key_weight,
        value_weight,
        out_weight,
        cache_key,
        cache_value,
        expert_gate,
        expert_up,
        expert_down,
        dense_gate,
        dense_up,
        dense_down,
    )


def solution(mesh):
    in_specs = (
        P("ep", "tp"),
        P(),
        P(None, "tp"),
        P(None, "tp"),
        P(None, "tp"),
        P(),
        P(),
        P("tp"),
        P(),
        P("tp", None),
        P("ep", None, "tp"),
        P("ep", None, "tp"),
        P("ep"),
        P("tp"),
        P("ep", None),
        P("ep", None),
        P("ep", None, "tp"),
        P("ep", None, "tp"),
        P("ep", "tp", None),
        P("tp", "ep"),
        P("tp", "ep"),
        P("ep", "tp"),
        P("tp"),
    )
    out_specs = (P("ep", "tp"), P("ep", "tp"), P("ep", "tp"))
    step = functools.partial(body, mesh.shape["ep"], mesh.shape["tp"])
    return jax.shard_map(step, mesh=mesh, in_specs=in_specs, out_specs=out_specs, check_vma=False)
```

```python
import functools
import math

import jax
import jax.numpy as jnp
from jax import lax
from jax.experimental import pallas as pl
from jax.experimental.pallas import tpu as pltpu
from jax.sharding import PartitionSpec as P

EPSILON = 1e-06
CLAMP_LIMIT = 7.0
SWISH_ALPHA = 1.702
OUT_SCALE = 0.2 + 0.6 * math.exp(-0.6)
F32 = jnp.float32
BF16 = jnp.bfloat16
MESH = pl.DeviceIdType.MESH


def dot(a, b):
    return jnp.dot(a, b, preferred_element_type=F32)


def group_rms(values, gain, group):
    lane = lax.broadcasted_iota(jnp.int32, values.shape, 1)
    squares = values * values
    scale = jnp.zeros_like(values)
    for g in range(values.shape[1] // group):
        inside = (lane >= g * group) & (lane < (g + 1) * group)
        total = jnp.sum(jnp.where(inside, squares, 0.0), axis=1, keepdims=True)
        scale = jnp.where(inside, lax.rsqrt(total / group + EPSILON), scale)
    return values * scale * gain


def hand_on(a_ref, b_ref, c_ref, a_out, b_out, c_out):
    a_out[...] = a_ref[...]
    b_out[...] = b_ref[...]
    c_out[...] = c_ref[...]


def layer_kernel(
    n_ep,
    n_tp,
    lam_ref,
    len_ref,
    hid_ref,
    gain_attn_ref,
    qg_ref,
    kg_ref,
    sub_ref,
    gain_mix_ref,
    branch_ref,
    ids_ref,
    logits_ref,
    wq_hbm,
    wk_hbm,
    wv_hbm,
    wo_hbm,
    ck_hbm,
    cv_hbm,
    eg_hbm,
    eu_hbm,
    ed_hbm,
    dg_hbm,
    du_hbm,
    dd_hbm,
    out_ref,
    key_ref,
    val_ref,
    wq,
    wk,
    wv,
    wo,
    ck,
    cv,
    eg,
    eu,
    ed,
    dgbuf,
    dubuf,
    dd,
    hbuf,
    gbuf,
    bbuf,
    vrow,
    hout,
    res,
    abuf,
    gath,
    ybuf,
    ysend,
    pbuf,
    sbuf,
    rbuf,
    lsem,
    tp_send,
    tp_recv,
    g_send,
    f_send,
    g_recv,
    p_sem,
    r_send,
    r_recv,
):
    e = lax.axis_index("ep")
    t = lax.axis_index("tp")
    chips = n_ep // 2
    chip = lax.div(e, 2)
    core = lax.rem(e, 2)
    sib = chip * 2 + (1 - core)
    n_all = chips * n_tp
    rows, half = hid_ref.shape
    width = half * n_tp

    loads = []
    for i, (src, dst) in enumerate(
        [
            (wq_hbm, wq),
            (wk_hbm, wk),
            (wv_hbm, wv),
            (ck_hbm, ck),
            (cv_hbm, cv),
            (wo_hbm, wo),
            (dg_hbm, dgbuf.at[t]),
            (du_hbm, dubuf.at[t]),
            (eg_hbm.at[0], eg),
            (eu_hbm.at[0], eu),
            (ed_hbm.at[0], ed),
            (dd_hbm, dd),
        ]
    ):
        copy = pltpu.make_async_copy(src, dst, lsem.at[i])
        copy.start()
        loads.append(copy)

    barrier = pltpu.get_barrier_semaphore()
    me = t * chips + chip

    def greet(i, carry):
        other = lax.rem(me + i, n_all)
        pl.semaphore_signal(
            barrier,
            inc=1,
            device_id={"ep": lax.rem(other, chips) * 2 + core, "tp": lax.div(other, chips)},
            device_id_type=MESH,
        )
        return carry

    lax.fori_loop(1, n_all, greet, 0)
    pl.semaphore_signal(barrier, inc=1, device_id={"ep": sib, "tp": t}, device_id_type=MESH)

    hbuf[t] = hid_ref[...]
    gbuf[t] = gain_mix_ref[...]
    bbuf[t] = branch_ref[...]

    ext = gath.shape[2] - width
    def split(table, first):
        high = table.astype(BF16).astype(F32)
        return jnp.where(first, high, table - high)

    logits = logits_ref[...]
    top = logits - jnp.max(logits, axis=0, keepdims=True)
    expo = jnp.exp(top)
    route = expo / jnp.sum(expo, axis=0, keepdims=True)
    ids = ids_ref[...]
    place = lax.broadcasted_iota(jnp.int32, (ext, rows), 0)
    place_id = jnp.where(place <= n_ep, place, place - (n_ep + 1))
    table = jnp.zeros((ext, rows), F32)
    for k in range(ids.shape[0]):
        table = table + jnp.where(place_id == ids[k : k + 1, :], route[k : k + 1, :], 0.0)
    table = split(table, place <= n_ep).astype(BF16)
    unit = lax.broadcasted_iota(jnp.int32, (rows, rows), 0) == lax.broadcasted_iota(
        jnp.int32, (rows, rows), 1
    )
    table = lax.dot_general(
        unit.astype(F32).astype(BF16), table, (((1,), (1,)), ((), ())), preferred_element_type=F32
    )

    pl.semaphore_wait(barrier, n_all)

    def tp_copies(kind, src, dst_ref):
        sends = []
        for d in range(1, n_tp):
            peer = lax.rem(t + d, n_tp)
            copy = pltpu.make_async_remote_copy(
                src_ref=src,
                dst_ref=dst_ref.at[t],
                send_sem=tp_send.at[kind, d - 1],
                recv_sem=tp_recv.at[kind, t],
                device_id={"ep": e, "tp": peer},
                device_id_type=MESH,
            )
            copy.start()
            sends.append(copy)
        return sends

    def tp_arrive(kind, src, dst_ref):
        for d in range(1, n_tp):
            peer = lax.rem(t + d, n_tp)
            pltpu.make_async_remote_copy(
                src_ref=src,
                dst_ref=dst_ref.at[peer],
                send_sem=tp_send.at[kind, d - 1],
                recv_sem=tp_recv.at[kind, peer],
                device_id={"ep": e, "tp": peer},
                device_id_type=MESH,
            ).wait_recv()

    pending = []
    pending += tp_copies(0, hid_ref, hbuf)
    pending += tp_copies(1, gain_mix_ref, gbuf)
    pending += tp_copies(2, branch_ref, bbuf)

    tp_arrive(0, hid_ref, hbuf)
    hidden = [hbuf[j].astype(F32) for j in range(n_tp)]
    square = sum(jnp.sum(h * h, axis=1, keepdims=True) for h in hidden)
    inverse = lax.rsqrt(square / width + EPSILON)
    normed = [
        (hidden[j] * inverse * gain_attn_ref[:, j * half : (j + 1) * half]).astype(BF16)
        for j in range(n_tp)
    ]

    def project(w):
        return sum(dot(normed[j], w[j * half : (j + 1) * half, :]) for j in range(n_tp))

    qk2 = qg_ref.shape[1]
    qk = qk2 // 2
    cols = wq.shape[1]
    heads = cols // qk2
    val = sub_ref.shape[1]
    q_gain = jnp.concatenate([qg_ref[...]] * heads, axis=1)
    k_gain = jnp.concatenate([kg_ref[...]] * heads, axis=1)
    sub_gain = jnp.concatenate([sub_ref[...]] * heads, axis=1)
    loads[0].wait()
    q_rows = group_rms(project(wq), q_gain, qk).astype(BF16).astype(F32)
    loads[1].wait()
    k_bf = group_rms(project(wk), k_gain, qk).astype(BF16)
    k_rows = k_bf.astype(F32)
    loads[2].wait()
    v_bf = project(wv).astype(BF16)
    key_ref[...] = k_bf
    val_ref[...] = v_bf
    vrow[...] = v_bf.astype(F32)

    qcol = lax.broadcasted_iota(jnp.int32, (16, cols), 1)
    qrow = lax.broadcasted_iota(jnp.int32, (16, cols), 0)
    inside = (qcol // qk) == (2 * (qrow % 8) + qrow // 8)
    vcol = lax.broadcasted_iota(jnp.int32, (8, heads * val), 1)
    vhead = lax.broadcasted_iota(jnp.int32, (8, heads * val), 0)
    own_head = (vcol // val) == vhead
    lrow = lax.broadcasted_iota(jnp.int32, (8, 1), 0)
    lam = jnp.zeros((8, 1), F32)
    for h in range(heads):
        lam = jnp.where(lrow == h, lam_ref[h], lam)
    factor = qk ** (-0.5)
    cache_len = ck.shape[1]
    pos = lax.broadcasted_iota(jnp.int32, (16, cache_len), 1)
    loads[3].wait()
    loads[4].wait()
    for s in range(rows):
        q_s = jnp.where(inside, q_rows[s : s + 1, :], 0.0)
        own = jnp.exp(jnp.sum(q_s * k_rows[s : s + 1, :], axis=1, keepdims=True) * factor)
        score = lax.dot_general(
            q_s.astype(BF16), ck[s], (((1,), (1,)), ((), ())), preferred_element_type=F32
        )
        past = jnp.where(pos < len_ref[s], jnp.exp(score * factor), 0.0)
        inv_den = 1.0 / (jnp.sum(past, axis=1, keepdims=True) + own)
        prob = past * inv_den
        own = own * inv_den
        weight = (prob[:8] - lam * prob[8:]).astype(BF16)
        weight_own = (own[:8] - lam * own[8:]).astype(BF16).astype(F32)
        mix = dot(weight, cv[s]) + weight_own * vrow[s : s + 1, :]
        mix = jnp.where(own_head, mix, 0.0)
        square = jnp.sum(mix * mix, axis=1, keepdims=True)
        mix = mix * lax.rsqrt(square / val + EPSILON) * sub_gain * OUT_SCALE
        hout[s : s + 1, :] = jnp.sum(mix, axis=0, keepdims=True)
    loads[5].wait()
    attn = dot(hout[...].astype(BF16), wo[...])
    abuf[t] = attn.astype(BF16)
    pending += tp_copies(3, abuf.at[t], abuf)
    loads[6].wait()
    loads[7].wait()
    pending += tp_copies(4, dgbuf.at[t], dgbuf)
    pending += tp_copies(5, dubuf.at[t], dubuf)
    tp_arrive(1, gain_mix_ref, gbuf)
    tp_arrive(2, branch_ref, bbuf)
    tp_arrive(3, abuf.at[t], abuf)

    for d in range(1, n_tp):
        attn = attn + abuf[lax.rem(t + d, n_tp)].astype(F32)
    slot = core * chips + chip
    square = jnp.zeros((rows, 1), F32)
    total = []
    for j in range(n_tp):
        r = hbuf[j].astype(F32) + attn[:, j * half : (j + 1) * half]
        res[j] = r
        total.append(r)
        square = square + jnp.sum(r * r, axis=1, keepdims=True)
    inverse = lax.rsqrt(square / width + EPSILON)
    logit = jnp.zeros((rows, 1), F32)
    for j in range(n_tp):
        m = total[j] * inverse * gbuf[j]
        logit = logit + jnp.sum(m * bbuf[j], axis=1, keepdims=True)
        gath[slot, :, j * half : (j + 1) * half] = m.astype(BF16)
    branch = 1.0 / (1.0 + jnp.exp(-logit))
    lane = lax.broadcasted_iota(jnp.int32, (rows, ext), 1)
    at_branch = (lane == n_ep) | (lane == 2 * n_ep + 1)
    table = jnp.where(at_branch, split(branch, lane <= n_ep), table)
    gath[slot, :, width:] = table.astype(BF16)

    def gather_copy(at, send, ep_to):
        return pltpu.make_async_remote_copy(
            src_ref=gath.at[at],
            dst_ref=gath.at[at],
            send_sem=send,
            recv_sem=g_recv.at[at],
            device_id={"ep": ep_to, "tp": t},
            device_id_type=MESH,
        )

    columns = chips // 2
    column = lax.div(chip, 2)
    side = lax.rem(chip, 2)
    beside = (column * 2 + (1 - side)) * 2 + core

    def scatter(i, carry):
        to = lax.rem(column + i, columns) * 2 + side
        gather_copy(slot, g_send.at[i], to * 2 + core).start()
        return carry

    lax.fori_loop(1, columns, scatter, 0)
    gather_copy(slot, f_send.at[0], beside).start()
    gather_copy(slot, f_send.at[columns], sib).start()

    def source(i, of_side):
        return core * chips + lax.rem(column + columns - i, columns) * 2 + of_side

    def forward(i, carry):
        at = source(i, side)
        gather_copy(at, f_send.at[i], beside).wait_recv()
        gather_copy(at, f_send.at[i], beside).start()
        gather_copy(at, f_send.at[columns + i], sib).start()
        return carry

    lax.fori_loop(1, columns, forward, 0)

    def forward_beside(i, carry):
        at = source(i, 1 - side)
        gather_copy(at, f_send.at[2 * columns + i], sib).wait_recv()
        gather_copy(at, f_send.at[2 * columns + i], sib).start()
        return carry

    lax.fori_loop(0, columns, forward_beside, 0)

    for i in range(8, 12):
        loads[i].wait()
    tp_arrive(4, dgbuf.at[t], dgbuf)
    tp_arrive(5, dubuf.at[t], dubuf)

    def expert(par):
        x = gath[pl.ds(par * chips, chips), :, :].reshape(chips * rows, width + ext)
        tokens = x[:, :width]
        extra = x[:, width:].astype(F32)
        place = lax.broadcasted_iota(jnp.int32, extra.shape, 1)
        mine = (place == e) | (place == e + n_ep + 1)
        w_route = jnp.sum(jnp.where(mine, extra, 0.0), axis=1, keepdims=True)
        dense_at = (place == n_ep) | (place == 2 * n_ep + 1)
        w_dense = jnp.sum(jnp.where(dense_at, extra, 0.0), axis=1, keepdims=True)
        gate = jnp.minimum(dot(tokens, eg[...]), CLAMP_LIMIT)
        up = jnp.clip(dot(tokens, eu[...]), -CLAMP_LIMIT, CLAMP_LIMIT)
        act = ((up + 1.0) * gate / (1.0 + jnp.exp(-SWISH_ALPHA * gate))).astype(BF16)
        dg = sum(dot(tokens[:, j * half : (j + 1) * half], dgbuf[j]) for j in range(n_tp))
        du = sum(dot(tokens[:, j * half : (j + 1) * half], dubuf[j]) for j in range(n_tp))
        dact = (dg / (1.0 + jnp.exp(-dg)) * du).astype(BF16)
        dense = dot(dact, dd[...]) * w_dense
        parts = []
        for j in range(n_tp):
            y = dot(act, ed[:, j * half : (j + 1) * half]) * w_route
            parts.append((y + jnp.where(t == j, dense, 0.0)).reshape(chips, rows, half))
        return parts

    own_parts = expert(core)
    for j in range(n_tp):
        ybuf[j] = own_parts[j]

    def arrived(i, carry):
        at = (1 - core) * chips + i
        gather_copy(at, f_send.at[0], sib).wait_recv()
        return carry

    lax.fori_loop(0, chips, arrived, 0)
    sib_parts = expert(1 - core)
    for j in range(n_tp):
        ysend[j] = sib_parts[j].astype(BF16)
    pair = pltpu.make_async_remote_copy(
        src_ref=ysend,
        dst_ref=pbuf,
        send_sem=p_sem.at[0],
        recv_sem=p_sem.at[1],
        device_id={"ep": sib, "tp": t},
        device_id_type=MESH,
    )
    pair.start()
    pair.wait_recv()
    for j in range(n_tp):
        both = ybuf[j] + pbuf[j].astype(F32)
        sbuf[j] = both.astype(BF16)

    def result_copy(i, to_t, to_chip, from_t, from_chip):
        return pltpu.make_async_remote_copy(
            src_ref=sbuf.at[to_t, to_chip],
            dst_ref=rbuf.at[from_t, from_chip],
            send_sem=r_send.at[i],
            recv_sem=r_recv.at[from_t * chips + from_chip],
            device_id={"ep": to_chip * 2 + core, "tp": to_t},
            device_id_type=MESH,
        )

    def give(i, carry):
        to = lax.rem(me + i, n_all)
        result_copy(i, lax.div(to, chips), lax.rem(to, chips), t, chip).start()
        return carry

    lax.fori_loop(1, n_all, give, 0)
    final = res[t] + ybuf[t, chip] + pbuf[t, chip].astype(F32)

    def take(i, total):
        src = lax.rem(me + n_all - i, n_all)
        src_t, src_chip = lax.div(src, chips), lax.rem(src, chips)
        result_copy(i, t, chip, src_t, src_chip).wait_recv()
        return total + rbuf[src_t, src_chip].astype(F32)

    final = lax.fori_loop(1, n_all, take, final)
    out_ref[...] = final.astype(BF16)

    for copy in pending:
        copy.wait_send()
    pair.wait_send()

    def drain_gather(i, carry):
        gather_copy(slot, g_send.at[i], sib).wait_send()
        return carry

    lax.fori_loop(1, columns, drain_gather, 0)

    def drain_forward(i, carry):
        gather_copy(slot, f_send.at[i], sib).wait_send()
        return carry

    lax.fori_loop(0, 3 * columns, drain_forward, 0)

    def drain_result(i, carry):
        to = lax.rem(me + i, n_all)
        result_copy(i, lax.div(to, chips), lax.rem(to, chips), t, chip).wait_send()
        return carry

    lax.fori_loop(1, n_all, drain_result, 0)


def body(
    n_ep,
    n_tp,
    hidden_in,
    norm_gain_attn,
    query_weight,
    key_weight,
    value_weight,
    query_gain,
    key_gain,
    lambda_head,
    sub_gain,
    out_weight,
    cache_key,
    cache_value,
    lengths,
    norm_gain_mix,
    route_ids,
    route_logits,
    expert_gate,
    expert_up,
    expert_down,
    dense_gate,
    dense_up,
    dense_down,
    branch_gate,
):
    rows, half = hidden_in.shape
    width = half * n_tp
    chips = n_ep // 2
    n_all = chips * n_tp
    ext = -(-2 * (n_ep + 1) // 128) * 128
    smem = pl.BlockSpec(memory_space=pltpu.SMEM)
    vmem = pl.BlockSpec(memory_space=pltpu.VMEM)
    hbm = pl.BlockSpec(memory_space=pl.ANY)
    dma = pltpu.SemaphoreType.DMA
    cols = query_weight.shape[1]
    vcols = value_weight.shape[1]
    block = (n_tp, chips, rows, half)
    scratch = [
        pltpu.VMEM(query_weight.shape, BF16),
        pltpu.VMEM(key_weight.shape, BF16),
        pltpu.VMEM(value_weight.shape, BF16),
        pltpu.VMEM(out_weight.shape, BF16),
        pltpu.VMEM(cache_key.shape, BF16),
        pltpu.VMEM(cache_value.shape, BF16),
        pltpu.VMEM(expert_gate.shape[1:], BF16),
        pltpu.VMEM(expert_up.shape[1:], BF16),
        pltpu.VMEM(expert_down.shape[1:], BF16),
        pltpu.VMEM((n_tp,) + dense_gate.shape, BF16),
        pltpu.VMEM((n_tp,) + dense_up.shape, BF16),
        pltpu.VMEM(dense_down.shape, BF16),
        pltpu.VMEM((n_tp, rows, half), BF16),
        pltpu.VMEM((n_tp, 1, half), F32),
        pltpu.VMEM((n_tp, 1, half), F32),
        pltpu.VMEM((rows, vcols), F32),
        pltpu.VMEM((rows, vcols), F32),
        pltpu.VMEM((n_tp, rows, half), F32),
        pltpu.VMEM((n_tp, rows, width), BF16),
        pltpu.VMEM((n_ep, rows, width + ext), BF16),
        pltpu.VMEM(block, F32),
        pltpu.VMEM(block, BF16),
        pltpu.VMEM(block, BF16),
        pltpu.VMEM(block, BF16),
        pltpu.VMEM(block, BF16),
        dma((12,)),
        dma((6, n_tp)),
        dma((6, n_tp)),
        dma((chips // 2,)),
        dma((3 * (chips // 2),)),
        dma((n_ep,)),
        dma((2,)),
        dma((n_all,)),
        dma((n_all,)),
    ]
    outs = pl.pallas_call(
        functools.partial(layer_kernel, n_ep, n_tp),
        out_shape=(
            jax.ShapeDtypeStruct((rows, half), BF16),
            jax.ShapeDtypeStruct((rows, cols), BF16),
            jax.ShapeDtypeStruct((rows, vcols), BF16),
        ),
        in_specs=[smem] * 2 + [vmem] * 9 + [hbm] * 12,
        out_specs=(vmem, vmem, vmem),
        scratch_shapes=scratch,
        compiler_params=pltpu.CompilerParams(
            collective_id=0, has_side_effects=True, vmem_limit_bytes=56 * 1024 * 1024
        ),
    )(
        lambda_head,
        lengths,
        hidden_in,
        norm_gain_attn.reshape(1, -1),
        query_gain.reshape(1, -1),
        key_gain.reshape(1, -1),
        sub_gain.reshape(1, -1),
        norm_gain_mix.reshape(1, -1),
        branch_gate.reshape(1, -1),
        route_ids.T,
        route_logits.T,
        query_weight,
        key_weight,
        value_weight,
        out_weight,
        cache_key,
        cache_value,
        expert_gate,
        expert_up,
        expert_down,
        dense_gate,
        dense_up,
        dense_down,
    )
    return pl.pallas_call(
        hand_on,
        out_shape=tuple(jax.ShapeDtypeStruct(o.shape, o.dtype) for o in outs),
        in_specs=[vmem] * 3,
        out_specs=(vmem, vmem, vmem),
    )(*outs)


def solution(mesh):
    in_specs = (
        P("ep", "tp"),
        P(),
        P(None, "tp"),
        P(None, "tp"),
        P(None, "tp"),
        P(),
        P(),
        P("tp"),
        P(),
        P("tp", None),
        P("ep", None, "tp"),
        P("ep", None, "tp"),
        P("ep"),
        P("tp"),
        P("ep", None),
        P("ep", None),
        P("ep", None, "tp"),
        P("ep", None, "tp"),
        P("ep", "tp", None),
        P("tp", "ep"),
        P("tp", "ep"),
        P("ep", "tp"),
        P("tp"),
    )
    out_specs = (P("ep", "tp"), P("ep", "tp"), P("ep", "tp"))
    step = functools.partial(body, mesh.shape["ep"], mesh.shape["tp"])
    return jax.shard_map(step, mesh=mesh, in_specs=in_specs, out_specs=out_specs, check_vma=False)
```
